32 devices in a mesh: sp: 16 (over z, y, x), tp: 2 (over core).
Axes of the slice: x: 2, y: 2, z: 4, core: 2. Of those that a mesh axis runs over, the one named last changes fastest.
Arguments:
- queries: bfloat16 [4096, 1024], P('sp', 'tp'), may hold values from -6 to 6
- keys: bfloat16 [4096, 256], P('sp'), may hold values from -6 to 6
- values: bfloat16 [4096, 256], P('sp'), may hold values from -6 to 6
- query_gain: float32 [128], replicated, may hold values from 1.4 to 5.5
- key_gain: float32 [128], replicated, may hold values from 1.4 to 5.5
- residual_in: bfloat16 [4096, 2048], P(('sp', 'tp')), may hold values from -6 to 6
- out_weight: bfloat16 [1024, 2048], P('tp'), may hold values from -0.1875 to 0.1875
- norm_gain: float32 [2048], replicated, may hold values from 0.1 to 1.9
- gate_weight: bfloat16 [2048, 3072], P('sp', 'tp'), may hold values from -0.125 to 0.125
- up_weight: bfloat16 [2048, 3072], P('sp', 'tp'), may hold values from -0.125 to 0.125
- down_weight: bfloat16 [3072, 2048], P('tp', 'sp'), may hold values from -0.109375 to 0.109375
Outputs:
- result: bfloat16 [4096, 2048], P(('sp', 'tp'))
The draws below stay inside these ranges and needn't reach their ends.
All inputs are finite; a program needn't handle non-finite values.
Results may differ from the reference program's by a relative error of at most 0.017.
Values may be sent and summed in bfloat16 or wider, within the bound.
A program may use at most 64 MiB of HBM per device.

```python
import math
import jax
import jax.numpy as jnp
from jax import lax

D = 2048
FF = 3072
HEAD = 128
Q_HEADS = 8
KV_HEADS = 2
GRID_WIDTH = 64
TOKENS = 4096
N_TP = 2


def raw_keys(key):
    drawn = jax.random.normal(jax.random.fold_in(key, 11), (TOKENS, KV_HEADS * HEAD), jnp.float32)
    return jnp.clip(drawn, -6.0, 6.0)


def draw_keys(key, part):
    return raw_keys(key).astype(jnp.bfloat16)


def draw_queries(key, part):
    background = jnp.clip(jax.random.normal(jax.random.fold_in(key, 12), (TOKENS, Q_HEADS * HEAD), jnp.float32), -6.0, 6.0)
    return background.astype(jnp.bfloat16)


def draw_values(key, part):
    offset = 1.5 * jax.random.normal(jax.random.fold_in(key, 31), (1, KV_HEADS * HEAD), jnp.float32)
    noise = jax.random.normal(jax.random.fold_in(key, 32), (TOKENS, KV_HEADS * HEAD), jnp.float32)
    return jnp.clip(offset + noise, -6.0, 6.0).astype(jnp.bfloat16)


def draw_gain(key, salt):
    return jax.random.uniform(jax.random.fold_in(key, salt), (HEAD,), jnp.float32, 1.4, 2.0)


def draw_query_gain(key, part):
    return draw_gain(key, 21)


def draw_key_gain(key, part):
    return draw_gain(key, 22)


def levels(stream_key, extent, cuts, smallest, high):
    factor_of, own = 1.0, jax.random.fold_in(stream_key, 6)
    for axis_at, parts in cuts:
        draws = jnp.exp(jax.random.uniform(jax.random.fold_in(own, axis_at), (parts,), jnp.float32, smallest / len(cuts), high / len(cuts)))
        factor_of = factor_of * jnp.repeat(draws, extent[axis_at] // parts).reshape([-1 if axis == axis_at else 1 for axis in range(len(extent))])
    return factor_of


def centred(own_key, extent, scale, most, cuts=(), kind=jnp.bfloat16):
    loudness = levels(own_key, extent, cuts, -0.22, 0.18) if cuts else 1.0
    entries = jax.random.normal(own_key, extent, jnp.float32) * scale * loudness
    return jnp.minimum(jnp.maximum(entries, -most), most).astype(kind)


def setup_inputs(seed: int = 0) -> dict:
    seeds = jax.random.split(jax.random.key(seed), 12)
    queries = draw_queries(jax.random.fold_in(seeds[11], 71), 0)
    keys = draw_keys(jax.random.fold_in(seeds[11], 71), 0)
    values = draw_values(jax.random.fold_in(seeds[11], 71), 0)
    query_gain = draw_query_gain(jax.random.fold_in(seeds[11], 71), 0)
    key_gain = draw_key_gain(jax.random.fold_in(seeds[11], 71), 0)
    residual_in = centred(seeds[5], (TOKENS, D), 1.0, 6.0, ((0, 32),))
    out_weight = centred(seeds[6], (Q_HEADS * HEAD, D), (Q_HEADS * HEAD) ** -0.5, 0.1875, ((0, 2),))
    norm_gain = jnp.clip(1.0 + 0.18 * jax.random.normal(seeds[7], (D,), jnp.float32), 0.1, 1.9)
    gate_weight = centred(seeds[8], (D, FF), D ** -0.5, 0.125, ((0, 16), (1, 2)))
    up_weight = centred(seeds[9], (D, FF), D ** -0.5, 0.125, ((0, 16), (1, 2)))
    down_weight = centred(seeds[10], (FF, D), FF ** -0.5, 0.109375, ((0, 2), (1, 16)))
    return {"queries": queries, "keys": keys, "values": values, "query_gain": query_gain, "key_gain": key_gain, "residual_in": residual_in, "out_weight": out_weight, "norm_gain": norm_gain, "gate_weight": gate_weight, "up_weight": up_weight, "down_weight": down_weight}


EPS = 1e-06
ROPE_BASE = 10000.0

def normalize(wide_values, gain):
    wide = wide_values.astype(jnp.float32)
    return wide * lax.rsqrt(lax.optimization_barrier(jnp.mean(wide * wide, axis=-1, keepdims=True)) + EPS) * gain.astype(jnp.float32)

def rotate_pair(segment, angles):
    half_size = segment.shape[-1] // 2
    first = segment[..., :half_size]
    second = segment[..., half_size:]
    cosine = jnp.cos(angles)[:, None, :]
    sine_part = jnp.sin(angles)[:, None, :]
    return jnp.concatenate([first * cosine - second * sine_part, second * cosine + first * sine_part], axis=-1)

def grid_rotary(head_rows, positions):
    head_size = head_rows.shape[-1]
    half_size = head_size // 2
    quarter = head_size // 4
    inverse = ROPE_BASE ** (-jnp.arange(quarter, dtype=jnp.float32) * 2.0 / half_size)
    row_angles = (positions // GRID_WIDTH).astype(jnp.float32)[:, None] * inverse
    col_angles = (positions % GRID_WIDTH).astype(jnp.float32)[:, None] * inverse
    return jnp.concatenate([rotate_pair(head_rows[..., :half_size], row_angles), rotate_pair(head_rows[..., half_size:], col_angles)], axis=-1)

def blockwise_sum(left, right, pieces):
    width = left.shape[1] // pieces

    def add_piece(total, index):
        start = (index * width).astype(jnp.int32)
        columns = lax.dynamic_slice_in_dim(left, start, width, 1)
        rows = lax.dynamic_slice_in_dim(right, start, width, 0)
        part = jnp.dot(columns, rows, preferred_element_type=jnp.float32)
        rounded = lax.optimization_barrier(part.astype(jnp.bfloat16)).astype(jnp.float32)
        return (total + rounded, None)
    start_total = jnp.zeros((left.shape[0], right.shape[1]), jnp.float32)
    total, unused = lax.scan(add_piece, start_total, jnp.arange(pieces, dtype=jnp.int32))
    return total

def reference(queries, keys, values, query_gain, key_gain, residual_in, out_weight, norm_gain, gate_weight, up_weight, down_weight):
    token_count = queries.shape[0]
    positions = jnp.arange(token_count, dtype=jnp.int32)
    group_size = Q_HEADS // KV_HEADS
    turned_queries = grid_rotary(normalize(queries.reshape(token_count, Q_HEADS, HEAD), query_gain), positions).astype(jnp.bfloat16)
    turned_keys = grid_rotary(normalize(keys.reshape(token_count, KV_HEADS, HEAD), key_gain), positions).astype(jnp.bfloat16)
    keys_wide = turned_keys.astype(jnp.float32)
    values_wide = values.reshape(token_count, KV_HEADS, HEAD).astype(jnp.float32)
    block_rows = math.gcd(token_count, 256)
    score_scale = HEAD ** (-0.5)

    def one_block(query_block):
        grouped = query_block.astype(jnp.float32).reshape(block_rows, KV_HEADS, group_size, HEAD)
        scores = jnp.einsum('bkgd,skd->kgbs', grouped, keys_wide) * score_scale
        peak_score = lax.optimization_barrier(jnp.max(scores, axis=-1, keepdims=True))
        raw = jnp.exp(scores - peak_score)
        weight_total = lax.optimization_barrier(jnp.sum(raw, axis=-1))
        rounded = lax.optimization_barrier(raw.astype(jnp.bfloat16)).astype(jnp.float32)
        summed = jnp.einsum('kgbs,skd->bkgd', rounded, values_wide)
        scaled = summed / jnp.transpose(weight_total, (2, 0, 1))[..., None]
        return scaled.reshape(block_rows, Q_HEADS * HEAD).astype(jnp.bfloat16)
    blocked = turned_queries.reshape(token_count // block_rows, block_rows, Q_HEADS, HEAD)
    attended = lax.map(one_block, blocked).reshape(token_count, Q_HEADS * HEAD)
    attention_out = blockwise_sum(attended, out_weight, N_TP)
    middle = (residual_in.astype(jnp.float32) + attention_out).astype(jnp.bfloat16)
    normed = normalize(middle, norm_gain).astype(jnp.bfloat16)
    gate_part = jnp.dot(normed, gate_weight, preferred_element_type=jnp.float32)
    lifted = jnp.dot(normed, up_weight, preferred_element_type=jnp.float32)
    hidden = (jax.nn.silu(gate_part) * lifted).astype(jnp.bfloat16)
    mixer_out = blockwise_sum(hidden, down_weight, N_TP)
    return (middle.astype(jnp.float32) + mixer_out).astype(jnp.bfloat16)
```

```python
import functools
import math

import jax
import jax.numpy as jnp
from jax import lax
from jax.experimental import pallas as pl
from jax.experimental.pallas import tpu as pltpu
from jax.sharding import PartitionSpec as P

Q_HEADS = 8
KV_HEADS = 2
GRID_WIDTH = 64


EPS = 1e-06
ROPE_BASE = 10000.0


def normalize(wide_values, gain):
    wide = wide_values.astype(jnp.float32)
    return wide * lax.rsqrt(jnp.mean(wide * wide, axis=-1, keepdims=True) + EPS) * gain


def rotate_pair(segment, angles):
    half_size = segment.shape[-1] // 2
    first = segment[..., :half_size]
    second = segment[..., half_size:]
    cosine = jnp.cos(angles)[:, None, :]
    sine_part = jnp.sin(angles)[:, None, :]
    return jnp.concatenate(
        [first * cosine - second * sine_part, second * cosine + first * sine_part], axis=-1
    )


def grid_rotary(head_rows, positions):
    head_size = head_rows.shape[-1]
    half_size = head_size // 2
    quarter = head_size // 4
    inverse = ROPE_BASE ** (-jnp.arange(quarter, dtype=jnp.float32) * 2.0 / half_size)
    row_angles = (positions // GRID_WIDTH).astype(jnp.float32)[:, None] * inverse
    col_angles = (positions % GRID_WIDTH).astype(jnp.float32)[:, None] * inverse
    return jnp.concatenate(
        [
            rotate_pair(head_rows[..., :half_size], row_angles),
            rotate_pair(head_rows[..., half_size:], col_angles),
        ],
        axis=-1,
    )


def gated(gate_part, lifted):
    return (jax.nn.silu(gate_part) * lifted).astype(jnp.bfloat16)


def local(
    queries,
    keys,
    values,
    query_gain,
    key_gain,
    residual_in,
    out_weight,
    norm_gain,
    gate_weight,
    up_weight,
    down_weight,
):
    tok_rows = queries.shape[0]
    head_size = query_gain.shape[0]
    local_heads = queries.shape[1] // head_size
    tp_index = lax.axis_index("tp")
    share = tok_rows // lax.axis_size("tp")
    positions = lax.axis_index("sp") * tok_rows + jnp.arange(tok_rows, dtype=jnp.int32)
    key_head = tp_index * local_heads // (Q_HEADS // KV_HEADS)
    own_keys = lax.dynamic_slice_in_dim(keys, key_head * head_size, head_size, 1)
    own_values = lax.dynamic_slice_in_dim(values, key_head * head_size, head_size, 1)
    turned_keys = grid_rotary(
        normalize(own_keys.reshape(tok_rows, 1, head_size), key_gain), positions
    )
    turned_keys = turned_keys.reshape(tok_rows, head_size).astype(jnp.bfloat16)
    turned_queries = grid_rotary(
        normalize(queries.reshape(tok_rows, local_heads, head_size), query_gain), positions
    )
    turned_queries = turned_queries.reshape(tok_rows * local_heads, head_size).astype(jnp.bfloat16)
    score_scale = head_size ** (-0.5)

    def attend_block(running, block_pair):
        peak_score, weight_total, weighted = running
        block_keys, block_values = block_pair
        scores = (
            lax.dot_general(
                turned_queries,
                block_keys,
                (((1,), (1,)), ((), ())),
                preferred_element_type=jnp.float32,
            )
            * score_scale
        )
        new_peak = jnp.maximum(peak_score, jnp.max(scores, axis=1))
        factor = jnp.exp(peak_score - new_peak)
        raw = jnp.exp(scores - new_peak[:, None])
        weight_total = weight_total * factor + jnp.sum(raw, axis=1)
        weighted = weighted * factor[:, None] + jnp.dot(
            raw.astype(jnp.bfloat16), block_values, preferred_element_type=jnp.float32
        )
        return ((new_peak, weight_total, weighted), None)

    row_count = tok_rows * local_heads
    start_carry = (
        jnp.full((row_count,), -1e30, jnp.float32),
        jnp.zeros((row_count,), jnp.float32),
        jnp.zeros((row_count, head_size), jnp.float32),
    )
    piece_keys = lax.all_gather(turned_keys, "sp", axis=0, tiled=True)
    piece_values = lax.all_gather(own_values, "sp", axis=0, tiled=True)
    span = math.gcd(piece_keys.shape[0], 512)
    blocks = piece_keys.shape[0] // span
    stacked = (
        piece_keys.reshape(blocks, span, head_size),
        piece_values.reshape(blocks, span, head_size),
    )
    updated, unused = lax.scan(attend_block, start_carry, stacked)
    peak_score, weight_total, weighted = updated
    attended = (
        (weighted / weight_total[:, None])
        .astype(jnp.bfloat16)
        .reshape(tok_rows, local_heads * head_size)
    )
    placed = lax.dynamic_update_slice_in_dim(
        jnp.zeros((tok_rows, residual_in.shape[1]), jnp.float32),
        residual_in.astype(jnp.float32),
        tp_index * share,
        0,
    )
    head_partial = jnp.dot(attended, out_weight, preferred_element_type=jnp.float32)
    partial_total, residual_rows = (
        lax.psum(head_partial.astype(jnp.bfloat16), "tp").astype(jnp.float32),
        lax.psum(placed.astype(jnp.bfloat16), "tp").astype(jnp.float32),
    )
    middle_rows = (residual_rows + partial_total).astype(jnp.bfloat16)
    normed = normalize(middle_rows, norm_gain).astype(jnp.bfloat16)
    middle = lax.dynamic_slice_in_dim(middle_rows, tp_index * share, share, 0)
    hidden_width = gate_weight.shape[1]
    side_by_side = jnp.concatenate(
        [
            lax.all_gather(gate_weight, "sp", axis=0, tiled=True),
            lax.all_gather(up_weight, "sp", axis=0, tiled=True),
        ],
        axis=1,
    )
    both_parts = jnp.dot(normed, side_by_side, preferred_element_type=jnp.float32)
    hidden = gated(both_parts[:, :hidden_width], both_parts[:, hidden_width:])
    partials = jnp.dot(
        hidden,
        lax.all_gather(down_weight, "sp", axis=1, tiled=True),
        preferred_element_type=jnp.float32,
    )
    mixer_out = lax.psum_scatter(
        partials.astype(jnp.bfloat16), "tp", scatter_dimension=0, tiled=True
    ).astype(jnp.float32)
    return (middle.astype(jnp.float32) + mixer_out).astype(jnp.bfloat16)


MESH = pl.DeviceIdType.MESH
MEMBERS = 4
LOG2E = 1.4426950408889634


def rotary_tables(tok_rows, head_size):
    positions = lax.axis_index("sp") * tok_rows + jnp.arange(tok_rows, dtype=jnp.int32)
    quarter = head_size // 4
    lane = jnp.arange(head_size)
    inverse = ROPE_BASE ** (-(lane % quarter).astype(jnp.float32) * 4.0 / head_size)
    row = (positions // GRID_WIDTH).astype(jnp.float32)[:, None]
    col = (positions % GRID_WIDTH).astype(jnp.float32)[:, None]
    angles = jnp.where(lane[None, :] < head_size // 2, row, col) * inverse[None, :]
    sign = jnp.where((lane // quarter) % 2 == 0, -1.0, 1.0)
    return jnp.cos(angles), jnp.sin(angles) * sign[None, :]


def layer_kernel(
    n_sp,
    queries,
    keys,
    values,
    query_gain,
    key_gain,
    residual_in,
    out_weight,
    norm_gain,
    gate_weight,
    up_weight,
    down_weight,
    cosine,
    sine,
    result,
    turned_q,
    key_buf,
    value_buf,
    peak,
    total,
    weighted,
    attended,
    head_send,
    head_own,
    head_recv,
    middle,
    tokens,
    gate_up,
    down,
    half_send,
    half_recv,
    share_send,
    share_recv,
    kv_send,
    kv_recv,
    w_send,
    w_recv,
    wf_send,
    wf_recv,
    h_send,
    h_recv,
    t_send,
    t_recv,
    o_send,
    o_recv,
):
    f32, bf16 = jnp.float32, jnp.bfloat16
    planes = n_sp // 4
    s = lax.axis_index("sp")
    t = lax.axis_index("tp")
    hi, mid, lo = s // 4, (s // 2) % 2, s % 2
    tok_rows, width = queries.shape
    head_size = query_gain.shape[1]
    heads = width // head_size
    share = residual_in.shape[0]
    model = residual_in.shape[1]
    depth = gate_weight.shape[0]
    part = gate_weight.shape[1] // MEMBERS
    sibling = {"sp": s, "tp": 1 - t}

    def at(hi_, mid_, lo_):
        return hi_ * 4 + mid_ * 2 + lo_

    def dev(sp_index):
        return {"sp": sp_index, "tp": t}

    x_peer = at(hi, mid, 1 - lo)
    y_peer = at(hi, 1 - mid, lo)

    def plane_peer(i):
        return at((hi + i % planes) % planes, mid, (lo + i // planes) % 2)

    def source_peer(i):
        return at((hi + planes - i % planes) % planes, mid, (lo + i // planes) % 2)

    def member(r):
        return at(hi - hi % 2 + (hi % 2 + r // 2) % 2, mid, (lo + r % 2) % 2)

    def remote(src, dst, ssem, rsem, device):
        return pltpu.make_async_remote_copy(
            src_ref=src, dst_ref=dst, send_sem=ssem, recv_sem=rsem,
            device_id=device, device_id_type=MESH,
        )

    barrier = pltpu.get_barrier_semaphore()
    for i in range(1, 2 * planes):
        pl.semaphore_signal(barrier, inc=1, device_id=dev(plane_peer(i)), device_id_type=MESH)
    pl.semaphore_signal(barrier, inc=1, device_id=dev(y_peer), device_id_type=MESH)
    pl.semaphore_signal(barrier, inc=1, device_id=sibling, device_id_type=MESH)

    quarter = head_size // 4
    lanes = lax.broadcasted_iota(jnp.int32, (tok_rows, head_size), 1)
    low_half = (lanes // quarter) % 2 == 0

    def turn(rows, gain):
        wide = rows.astype(f32)
        wide = wide * lax.rsqrt(jnp.mean(wide * wide, axis=-1, keepdims=True) + EPS) * gain
        partner = jnp.where(
            low_half, pltpu.roll(wide, head_size - quarter, 1), pltpu.roll(wide, quarter, 1)
        )
        return (wide * cosine[...] + partner * sine[...]).astype(bf16)

    key_head = (t * heads) // (Q_HEADS // KV_HEADS)
    kv_cols = pl.ds(pl.multiple_of(key_head * head_size, head_size), head_size)
    key_buf[0] = turn(keys[:, kv_cols], key_gain[...])
    value_buf[0] = values[:, kv_cols].astype(f32).T.astype(bf16)
    pl.semaphore_wait(barrier, 2 * planes + 1)

    def key_copy(src, dst, hop, device):
        return remote(key_buf.at[src], key_buf.at[dst], kv_send.at[0, hop, src], kv_recv.at[0, dst], device)

    def value_copy(src, dst, hop, device):
        return remote(value_buf.at[src], value_buf.at[dst], kv_send.at[1, hop, src], kv_recv.at[1, dst], device)

    def z_copies(d):
        device = dev(at((hi + d) % planes, mid, lo))
        return [key_copy_z(d, device), value_copy_z(d, device)]

    def key_copy_z(d, device):
        return remote(key_buf.at[0], key_buf.at[d], kv_send.at[0, 2, d], kv_recv.at[0, d], device)

    def value_copy_z(d, device):
        return remote(value_buf.at[0], value_buf.at[d], kv_send.at[1, 2, d], kv_recv.at[1, d], device)

    def first_copies(d):
        return [
            key_copy(d, planes + d, 0, dev(x_peer)),
            value_copy(d, 2 * planes + d, 1, dev(y_peer)),
            key_copy(d, 2 * planes + d, 1, dev(y_peer)),
            value_copy(d, planes + d, 0, dev(x_peer)),
        ]

    def second_copies(d):
        return [
            key_copy(planes + d, 3 * planes + d, 1, dev(y_peer)),
            value_copy(2 * planes + d, 3 * planes + d, 0, dev(x_peer)),
        ]

    def member_of(sp_index):
        return sp_index % 2 + 2 * ((sp_index // 4) % 2)

    def weight_refs(sp_index):
        rows = pl.ds(pl.multiple_of(sp_index * depth, depth), depth)
        return [
            gate_up.at[rows, pl.ds(0, part)],
            gate_up.at[rows, pl.ds(part, part)],
            down.at[:, rows],
        ]

    def own_refs(target):
        cols = pl.ds(pl.multiple_of(member_of(target) * part, part), part)
        return [gate_weight.at[:, cols], up_weight.at[:, cols], down_weight.at[cols, :]]

    def weight_copies(i):
        target = plane_peer(i)
        return [
            remote(a, b, w_send.at[k, i], w_recv.at[k, i], dev(target))
            for k, (a, b) in enumerate(zip(own_refs(target), weight_refs(s)))
        ]

    def forward_copies(i):
        source = source_peer(i)
        return [
            remote(a, a, wf_send.at[k, i], wf_recv.at[k, i], dev(y_peer))
            for k, a in enumerate(weight_refs(source))
        ]

    def own_forward():
        return [
            remote(a, b, wf_send.at[k, 0], wf_recv.at[k, 0], dev(y_peer))
            for k, (a, b) in enumerate(zip(own_refs(s), weight_refs(s)))
        ]

    def start(copies):
        for copy in copies:
            copy.start()

    def wait_recv(copies):
        for copy in copies:
            copy.wait_recv()

    def wait_send(copies):
        for copy in copies:
            copy.wait_send()

    def relay_weights(i):
        wait_recv(weight_copies(i))
        start(forward_copies(i))

    for d in range(1, planes):
        start(z_copies(d))
    start(first_copies(0))
    for i in range(1, planes):
        start(weight_copies(i))

    for a, b in zip(own_refs(s), weight_refs(s)):
        b[...] = a[...]
    for h in range(heads):
        turned_q[h] = turn(queries[:, h * head_size : (h + 1) * head_size], query_gain[...])
    peak[...] = jnp.full(peak.shape, -1e30, f32)
    total[...] = jnp.zeros(total.shape, f32)
    weighted[...] = jnp.zeros(weighted.shape, f32)
    exponent_scale = head_size ** (-0.5) * LOG2E

    def attend(slot):
        block_keys = key_buf[slot]
        block_values = value_buf[slot]
        for h in range(heads):
            scores = lax.dot_general(
                block_keys, turned_q[h], (((1,), (1,)), ((), ())), preferred_element_type=f32
            )
            old_peak = peak[h]
            new_peak = jnp.maximum(old_peak, jnp.max(scores, axis=0, keepdims=True))
            factor = jnp.exp2((old_peak - new_peak) * exponent_scale)
            raw = jnp.exp2((scores - new_peak) * exponent_scale)
            total[h] = total[h] * factor + jnp.sum(raw, axis=0, keepdims=True)
            weighted[h] = weighted[h] * factor + jnp.dot(
                block_values, raw.astype(bf16), preferred_element_type=f32
            )
            peak[h] = new_peak

    def first_step(d, carry):
        wait_recv(z_copies(d))
        start(first_copies(d))
        return carry

    def second_step(d, carry):
        wait_recv([first_copies(d)[0], first_copies(d)[1]])
        start(second_copies(d))
        return carry

    def attend_step(slot, carry):
        attend(slot)
        return carry

    attend(0)
    lax.fori_loop(1, planes, first_step, 0)
    lax.fori_loop(1, planes, attend_step, 0)
    lax.fori_loop(0, planes, second_step, 0)
    start(own_forward())
    for i in range(planes, 2 * planes):
        start(weight_copies(i))

    def third_step(d, carry):
        first_copies(d)[3].wait_recv()
        attend(planes + d)
        return carry

    def fourth_step(d, carry):
        first_copies(d)[2].wait_recv()
        attend(2 * planes + d)
        return carry

    def fifth_step(d, carry):
        wait_recv(second_copies(d))
        attend(3 * planes + d)

        @pl.when(d > 0)
        def _():
            relay_weights(d)

        return carry

    lax.fori_loop(0, planes, third_step, 0)
    lax.fori_loop(0, planes, fourth_step, 0)
    lax.fori_loop(0, planes, fifth_step, 0)
    for h in range(heads):
        attended[:, h * head_size : (h + 1) * head_size] = (weighted[h] / total[h]).T.astype(bf16)

    own_rows = pl.ds(pl.multiple_of(t * share, share), share)
    other_rows = pl.ds(pl.multiple_of((1 - t) * share, share), share)
    head_send[...] = jnp.dot(
        attended[other_rows, :], out_weight[...], preferred_element_type=f32
    ).astype(bf16)
    head_copy = remote(head_send, head_recv, h_send, h_recv, sibling)
    head_copy.start()
    head_own[...] = jnp.dot(
        attended[own_rows, :], out_weight[...], preferred_element_type=f32
    ).astype(bf16)
    head_copy.wait_recv()
    added = head_own[...].astype(f32) + head_recv[...].astype(f32)
    middle[...] = (residual_in[...].astype(f32) + added).astype(bf16)
    wide = middle[...].astype(f32)
    tokens[0, t] = (
        wide * lax.rsqrt(jnp.mean(wide * wide, axis=-1, keepdims=True) + EPS) * norm_gain[...]
    ).astype(bf16)

    def token_copy(r):
        return remote(
            tokens.at[0, t], tokens.at[r, t], t_send.at[0, r], t_recv.at[0, r], dev(member(r))
        )

    def sibling_copy(r):
        return remote(
            tokens.at[r, t], tokens.at[r, t], t_send.at[1, r], t_recv.at[1, r], sibling
        )

    def sibling_arrival(r):
        return remote(
            tokens.at[r, 1 - t], tokens.at[r, 1 - t], t_send.at[1, r], t_recv.at[1, r], sibling
        )

    for r in range(1, MEMBERS):
        token_copy(r).start()
    sibling_copy(0).start()

    def relay_step(i, carry):
        relay_weights(i)
        return carry

    lax.fori_loop(planes, 2 * planes, relay_step, 0)
    for r in range(1, MEMBERS):
        token_copy(r).wait_recv()
        sibling_copy(r).start()

    def arrive_step(i, carry):
        wait_recv(
            [
                remote(a, a, wf_send.at[k, i], wf_recv.at[k, i], dev(y_peer))
                for k, a in enumerate(weight_refs(source_peer(i) + 2 - 4 * mid))
            ]
        )
        return carry

    lax.fori_loop(0, 2 * planes, arrive_step, 0)

    def half_copy(r):
        return remote(
            half_send.at[r], half_recv.at[r], o_send.at[0, r], o_recv.at[0, r], sibling
        )

    def share_copy(r):
        return remote(
            share_send.at[r], share_recv.at[r], o_send.at[1, r], o_recv.at[1, r], dev(member(r))
        )

    def mix_step(step, carry):
        r = (step + 1) % MEMBERS
        sibling_arrival(r).wait_recv()
        rows = tokens[r].reshape(2 * share, model)
        both = jnp.dot(rows, gate_up[...], preferred_element_type=f32)
        hidden = gated(both[:, :part], both[:, part:])
        attended[:, 0:part] = hidden
        half_send[r] = jnp.dot(
            attended[other_rows, 0:part], down[...], preferred_element_type=f32
        ).astype(bf16)
        half_copy(r).start()
        partial = jnp.dot(attended[own_rows, 0:part], down[...], preferred_element_type=f32)
        half_copy(r).wait_recv()
        share_send[r] = (partial + half_recv[r].astype(f32)).astype(bf16)

        @pl.when(r > 0)
        def _():
            share_copy(r).start()

        return carry

    lax.fori_loop(0, MEMBERS, mix_step, 0)
    out = middle[...].astype(f32) + share_send[0].astype(f32)
    for r in range(1, MEMBERS):
        share_copy(r).wait_recv()
        out = out + share_recv[r].astype(f32)
    result[...] = out.astype(bf16)

    for d in range(1, planes):
        wait_send(z_copies(d))
    for d in range(planes):
        wait_send(first_copies(d))
        wait_send(second_copies(d))
    wait_send(own_forward())
    for i in range(1, 2 * planes):
        wait_send(weight_copies(i))
        wait_send(forward_copies(i))
    head_copy.wait_send()
    for r in range(MEMBERS):
        sibling_copy(r).wait_send()
        half_copy(r).wait_send()
        if r > 0:
            token_copy(r).wait_send()
            share_copy(r).wait_send()


def fused(
    queries, keys, values, query_gain, key_gain, residual_in, out_weight, norm_gain,
    gate_weight, up_weight, down_weight,
):
    n_sp = lax.axis_size("sp")
    planes = n_sp // 4
    tok_rows, width = queries.shape
    head_size = query_gain.shape[0]
    heads = width // head_size
    share, model = residual_in.shape
    part = gate_weight.shape[1] // MEMBERS
    f32, bf16 = jnp.float32, jnp.bfloat16
    cosine, sine = rotary_tables(tok_rows, head_size)
    vmem = pl.BlockSpec(memory_space=pltpu.VMEM)
    dma = pltpu.SemaphoreType.DMA
    return pl.pallas_call(
        functools.partial(layer_kernel, n_sp),
        out_shape=jax.ShapeDtypeStruct((share, model), bf16),
        in_specs=[vmem] * 13,
        out_specs=vmem,
        scratch_shapes=[
            pltpu.VMEM((heads, tok_rows, head_size), bf16),
            pltpu.VMEM((n_sp, tok_rows, head_size), bf16),
            pltpu.VMEM((n_sp, head_size, tok_rows), bf16),
            pltpu.VMEM((heads, 1, tok_rows), f32),
            pltpu.VMEM((heads, 1, tok_rows), f32),
            pltpu.VMEM((heads, head_size, tok_rows), f32),
            pltpu.VMEM((tok_rows, max(width, part)), bf16),
            pltpu.VMEM((share, model), bf16),
            pltpu.VMEM((share, model), bf16),
            pltpu.VMEM((share, model), bf16),
            pltpu.VMEM((share, model), bf16),
            pltpu.VMEM((MEMBERS, 2, share, model), bf16),
            pltpu.VMEM((model, 2 * part), bf16),
            pltpu.VMEM((part, model), bf16),
            pltpu.VMEM((MEMBERS, share, model), bf16),
            pltpu.VMEM((MEMBERS, share, model), bf16),
            pltpu.VMEM((MEMBERS, share, model), bf16),
            pltpu.VMEM((MEMBERS, share, model), bf16),
            dma((2, 3, n_sp)),
            dma((2, n_sp)),
            dma((3, 2 * planes)),
            dma((3, 2 * planes)),
            dma((3, 2 * planes)),
            dma((3, 2 * planes)),
            dma,
            dma,
            dma((2, MEMBERS)),
            dma((2, MEMBERS)),
            dma((2, MEMBERS)),
            dma((2, MEMBERS)),
        ],
        compiler_params=pltpu.CompilerParams(
            collective_id=0, has_side_effects=True, vmem_limit_bytes=60 * 1024 * 1024
        ),
    )(
        queries, keys, values, query_gain.reshape(1, -1), key_gain.reshape(1, -1), residual_in,
        out_weight, norm_gain.reshape(1, -1), gate_weight, up_weight, down_weight, cosine, sine,
    )


def layer(*args):
    queries, residual_in, gate_weight = args[0], args[5], args[8]
    head_size = args[3].shape[0]
    fits = (
        lax.axis_size("sp") % 8 == 0
        and lax.axis_size("tp") == 2
        and residual_in.shape[0] * 2 == queries.shape[0]
        and residual_in.shape[0] % 16 == 0
        and head_size == 128
        and queries.shape[1] % head_size == 0
        and gate_weight.shape[0] % 128 == 0
        and gate_weight.shape[1] % (128 * MEMBERS) == 0
        and (Q_HEADS // KV_HEADS) % (queries.shape[1] // head_size) == 0
    )
    return fused(*args) if fits else local(*args)


def solution(mesh):
    return jax.shard_map(
        layer,
        mesh=mesh,
        in_specs=(
            P("sp", "tp"),
            P("sp", None),
            P("sp", None),
            P(),
            P(),
            P(("sp", "tp"), None),
            P("tp", None),
            P(),
            P("sp", "tp"),
            P("sp", "tp"),
            P("tp", "sp"),
        ),
        out_specs=P(("sp", "tp"), None),
        check_vma=False,
    )
```

```python
import functools
import math

import jax
import jax.numpy as jnp
from jax import lax
from jax.experimental import pallas as pl
from jax.experimental.pallas import tpu as pltpu
from jax.sharding import PartitionSpec as P

Q_HEADS = 8
KV_HEADS = 2
GRID_WIDTH = 64


EPS = 1e-06
ROPE_BASE = 10000.0


def normalize(wide_values, gain):
    wide = wide_values.astype(jnp.float32)
    return wide * lax.rsqrt(jnp.mean(wide * wide, axis=-1, keepdims=True) + EPS) * gain


def rotate_pair(segment, angles):
    half_size = segment.shape[-1] // 2
    first = segment[..., :half_size]
    second = segment[..., half_size:]
    cosine = jnp.cos(angles)[:, None, :]
    sine_part = jnp.sin(angles)[:, None, :]
    return jnp.concatenate(
        [first * cosine - second * sine_part, second * cosine + first * sine_part], axis=-1
    )


def grid_rotary(head_rows, positions):
    head_size = head_rows.shape[-1]
    half_size = head_size // 2
    quarter = head_size // 4
    inverse = ROPE_BASE ** (-jnp.arange(quarter, dtype=jnp.float32) * 2.0 / half_size)
    row_angles = (positions // GRID_WIDTH).astype(jnp.float32)[:, None] * inverse
    col_angles = (positions % GRID_WIDTH).astype(jnp.float32)[:, None] * inverse
    return jnp.concatenate(
        [
            rotate_pair(head_rows[..., :half_size], row_angles),
            rotate_pair(head_rows[..., half_size:], col_angles),
        ],
        axis=-1,
    )


def gated(gate_part, lifted):
    return (jax.nn.silu(gate_part) * lifted).astype(jnp.bfloat16)


def local(
    queries,
    keys,
    values,
    query_gain,
    key_gain,
    residual_in,
    out_weight,
    norm_gain,
    gate_weight,
    up_weight,
    down_weight,
):
    tok_rows = queries.shape[0]
    head_size = query_gain.shape[0]
    local_heads = queries.shape[1] // head_size
    tp_index = lax.axis_index("tp")
    share = tok_rows // lax.axis_size("tp")
    positions = lax.axis_index("sp") * tok_rows + jnp.arange(tok_rows, dtype=jnp.int32)
    key_head = tp_index * local_heads // (Q_HEADS // KV_HEADS)
    own_keys = lax.dynamic_slice_in_dim(keys, key_head * head_size, head_size, 1)
    own_values = lax.dynamic_slice_in_dim(values, key_head * head_size, head_size, 1)
    turned_keys = grid_rotary(
        normalize(own_keys.reshape(tok_rows, 1, head_size), key_gain), positions
    )
    turned_keys = turned_keys.reshape(tok_rows, head_size).astype(jnp.bfloat16)
    turned_queries = grid_rotary(
        normalize(queries.reshape(tok_rows, local_heads, head_size), query_gain), positions
    )
    turned_queries = turned_queries.reshape(tok_rows * local_heads, head_size).astype(jnp.bfloat16)
    score_scale = head_size ** (-0.5)

    def attend_block(running, block_pair):
        peak_score, weight_total, weighted = running
        block_keys, block_values = block_pair
        scores = (
            lax.dot_general(
                turned_queries,
                block_keys,
                (((1,), (1,)), ((), ())),
                preferred_element_type=jnp.float32,
            )
            * score_scale
        )
        new_peak = jnp.maximum(peak_score, jnp.max(scores, axis=1))
        factor = jnp.exp(peak_score - new_peak)
        raw = jnp.exp(scores - new_peak[:, None])
        weight_total = weight_total * factor + jnp.sum(raw, axis=1)
        weighted = weighted * factor[:, None] + jnp.dot(
            raw.astype(jnp.bfloat16), block_values, preferred_element_type=jnp.float32
        )
        return ((new_peak, weight_total, weighted), None)

    row_count = tok_rows * local_heads
    start_carry = (
        jnp.full((row_count,), -1e30, jnp.float32),
        jnp.zeros((row_count,), jnp.float32),
        jnp.zeros((row_count, head_size), jnp.float32),
    )
    piece_keys = lax.all_gather(turned_keys, "sp", axis=0, tiled=True)
    piece_values = lax.all_gather(own_values, "sp", axis=0, tiled=True)
    span = math.gcd(piece_keys.shape[0], 512)
    blocks = piece_keys.shape[0] // span
    stacked = (
        piece_keys.reshape(blocks, span, head_size),
        piece_values.reshape(blocks, span, head_size),
    )
    updated, unused = lax.scan(attend_block, start_carry, stacked)
    peak_score, weight_total, weighted = updated
    attended = (
        (weighted / weight_total[:, None])
        .astype(jnp.bfloat16)
        .reshape(tok_rows, local_heads * head_size)
    )
    placed = lax.dynamic_update_slice_in_dim(
        jnp.zeros((tok_rows, residual_in.shape[1]), jnp.float32),
        residual_in.astype(jnp.float32),
        tp_index * share,
        0,
    )
    head_partial = jnp.dot(attended, out_weight, preferred_element_type=jnp.float32)
    partial_total, residual_rows = (
        lax.psum(head_partial.astype(jnp.bfloat16), "tp").astype(jnp.float32),
        lax.psum(placed.astype(jnp.bfloat16), "tp").astype(jnp.float32),
    )
    middle_rows = (residual_rows + partial_total).astype(jnp.bfloat16)
    normed = normalize(middle_rows, norm_gain).astype(jnp.bfloat16)
    middle = lax.dynamic_slice_in_dim(middle_rows, tp_index * share, share, 0)
    hidden_width = gate_weight.shape[1]
    side_by_side = jnp.concatenate(
        [
            lax.all_gather(gate_weight, "sp", axis=0, tiled=True),
            lax.all_gather(up_weight, "sp", axis=0, tiled=True),
        ],
        axis=1,
    )
    both_parts = jnp.dot(normed, side_by_side, preferred_element_type=jnp.float32)
    hidden = gated(both_parts[:, :hidden_width], both_parts[:, hidden_width:])
    partials = jnp.dot(
        hidden,
        lax.all_gather(down_weight, "sp", axis=1, tiled=True),
        preferred_element_type=jnp.float32,
    )
    mixer_out = lax.psum_scatter(
        partials.astype(jnp.bfloat16), "tp", scatter_dimension=0, tiled=True
    ).astype(jnp.float32)
    return (middle.astype(jnp.float32) + mixer_out).astype(jnp.bfloat16)


MESH = pl.DeviceIdType.MESH
MEMBERS = 4
LOG2E = 1.4426950408889634


def rotary_tables(tok_rows, head_size):
    positions = lax.axis_index("sp") * tok_rows + jnp.arange(tok_rows, dtype=jnp.int32)
    quarter = head_size // 4
    lane = jnp.arange(head_size)
    inverse = ROPE_BASE ** (-(lane % quarter).astype(jnp.float32) * 4.0 / head_size)
    row = (positions // GRID_WIDTH).astype(jnp.float32)[:, None]
    col = (positions % GRID_WIDTH).astype(jnp.float32)[:, None]
    angles = jnp.where(lane[None, :] < head_size // 2, row, col) * inverse[None, :]
    sign = jnp.where((lane // quarter) % 2 == 0, -1.0, 1.0)
    return jnp.cos(angles), jnp.sin(angles) * sign[None, :]


def layer_kernel(
    n_sp,
    queries,
    keys,
    values,
    query_gain,
    key_gain,
    residual_in,
    out_weight,
    norm_gain,
    gate_weight,
    up_weight,
    down_weight,
    cosine,
    sine,
    result,
    turned_q,
    key_buf,
    value_buf,
    peak,
    total,
    weighted,
    attended,
    head_send,
    head_own,
    head_recv,
    middle,
    tokens,
    gate_up,
    down,
    stage_gate_up,
    stage_down,
    half_send,
    half_recv,
    share_send,
    share_recv,
    share_own,
    kv_send,
    kv_recv,
    w_send,
    w_recv,
    wf_send,
    wf_recv,
    x_send,
    x_recv,
    h_send,
    h_recv,
    t_send,
    t_recv,
    o_send,
    o_recv,
):
    f32, bf16 = jnp.float32, jnp.bfloat16
    planes = n_sp // 4
    s = lax.axis_index("sp")
    t = lax.axis_index("tp")
    hi, mid, lo = s // 4, (s // 2) % 2, s % 2
    tok_rows, width = queries.shape
    head_size = query_gain.shape[1]
    heads = width // head_size
    share = residual_in.shape[0]
    model = residual_in.shape[1]
    depth = gate_weight.shape[0]
    part = gate_weight.shape[1] // MEMBERS
    sibling = {"sp": s, "tp": 1 - t}

    def at(hi_, mid_, lo_):
        return hi_ * 4 + mid_ * 2 + lo_

    def dev(sp_index):
        return {"sp": sp_index, "tp": t}

    x_peer = at(hi, mid, 1 - lo)
    y_peer = at(hi, 1 - mid, lo)

    def plane(d, sign):
        return (hi // 2 + planes + sign * (d // 2)) % (planes // 2) * 2 + (hi + d) % 2

    def plane_peer(i):
        return at(plane(i % planes, 1), mid, (lo + i // planes) % 2)

    def source_peer(i):
        return at(plane(i % planes, -1), mid, (lo + i // planes) % 2)

    def member(r):
        return at(hi - hi % 2 + (hi % 2 + r // 2) % 2, mid, (lo + r % 2) % 2)

    def remote(src, dst, ssem, rsem, device):
        return pltpu.make_async_remote_copy(
            src_ref=src, dst_ref=dst, send_sem=ssem, recv_sem=rsem,
            device_id=device, device_id_type=MESH,
        )

    barrier = pltpu.get_barrier_semaphore()
    for i in range(1, 2 * planes):
        pl.semaphore_signal(barrier, inc=1, device_id=dev(plane_peer(i)), device_id_type=MESH)
    pl.semaphore_signal(barrier, inc=1, device_id=dev(y_peer), device_id_type=MESH)
    pl.semaphore_signal(barrier, inc=1, device_id=sibling, device_id_type=MESH)

    quarter = head_size // 4
    lanes = lax.broadcasted_iota(jnp.int32, (tok_rows, head_size), 1)
    low_half = (lanes // quarter) % 2 == 0

    def turn(rows, gain):
        wide = rows.astype(f32)
        wide = wide * lax.rsqrt(jnp.mean(wide * wide, axis=-1, keepdims=True) + EPS) * gain
        partner = jnp.where(
            low_half, pltpu.roll(wide, head_size - quarter, 1), pltpu.roll(wide, quarter, 1)
        )
        return (wide * cosine[...] + partner * sine[...]).astype(bf16)

    key_head = (t * heads) // (Q_HEADS // KV_HEADS)
    kv_cols = pl.ds(pl.multiple_of(key_head * head_size, head_size), head_size)
    key_buf[0] = turn(keys[:, kv_cols], key_gain[...])
    value_buf[0] = values[:, kv_cols].astype(f32).T.astype(bf16)
    pl.semaphore_wait(barrier, 2 * planes + 1)

    def key_copy(src, dst, hop, device):
        return remote(key_buf.at[src], key_buf.at[dst], kv_send.at[0, hop, src], kv_recv.at[0, dst], device)

    def value_copy(src, dst, hop, device):
        return remote(value_buf.at[src], value_buf.at[dst], kv_send.at[1, hop, src], kv_recv.at[1, dst], device)

    def z_copies(d):
        device = dev(at(plane(d, 1), mid, lo))
        return [key_copy_z(d, device), value_copy_z(d, device)]

    def key_copy_z(d, device):
        return remote(key_buf.at[0], key_buf.at[d], kv_send.at[0, 2, d], kv_recv.at[0, d], device)

    def value_copy_z(d, device):
        return remote(value_buf.at[0], value_buf.at[d], kv_send.at[1, 2, d], kv_recv.at[1, d], device)

    def first_copies(d):
        return [
            key_copy(d, planes + d, 0, dev(x_peer)),
            value_copy(d, 2 * planes + d, 1, dev(y_peer)),
            key_copy(d, 2 * planes + d, 1, dev(y_peer)),
            value_copy(d, planes + d, 0, dev(x_peer)),
        ]

    def second_copies(d):
        return [
            key_copy(planes + d, 3 * planes + d, 1, dev(y_peer)),
            value_copy(2 * planes + d, 3 * planes + d, 0, dev(x_peer)),
        ]

    def member_of(sp_index):
        return sp_index % 2 + 2 * ((sp_index // 4) % 2)

    def weight_refs(sp_index):
        rows = pl.ds(pl.multiple_of(sp_index * depth, depth), depth)
        return [
            gate_up.at[rows, pl.ds(0, part)],
            gate_up.at[rows, pl.ds(part, part)],
            down.at[:, rows],
        ]

    def own_refs(target):
        cols = pl.ds(pl.multiple_of(member_of(target) * part, part), part)
        return [gate_weight.at[:, cols], up_weight.at[:, cols], down_weight.at[cols, :]]

    def weight_copies(i):
        target = plane_peer(i)
        return [
            remote(a, b, w_send.at[k, i], w_recv.at[k, i], dev(target))
            for k, (a, b) in enumerate(zip(own_refs(target), weight_refs(s)))
        ]

    def forward_copies(i):
        source = source_peer(i)
        return [
            remote(a, a, wf_send.at[k, i], wf_recv.at[k, i], dev(y_peer))
            for k, a in enumerate(weight_refs(source))
        ]

    def own_forward():
        return [
            remote(a, b, wf_send.at[k, 0], wf_recv.at[k, 0], dev(y_peer))
            for k, (a, b) in enumerate(zip(own_refs(s), weight_refs(s)))
        ]

    def stage_refs(b):
        return [
            stage_gate_up.at[b, :, pl.ds(0, part)],
            stage_gate_up.at[b, :, pl.ds(part, part)],
            stage_down.at[b],
        ]

    def stage_copies(b):
        return [
            remote(a, c, x_send.at[k, b], x_recv.at[k, b], dev(x_peer))
            for k, (a, c) in enumerate(zip(own_refs(4 * b + 1 - lo), stage_refs(b)))
        ]

    def onward_copies(d):
        target = plane_peer(d)
        return [
            remote(a, c, w_send.at[k, planes + d], w_recv.at[k, planes + d], dev(target))
            for k, (a, c) in enumerate(zip(stage_refs((hi + d) % 2), weight_refs(x_peer)))
        ]

    def stage_forward():
        return [
            remote(a, c, wf_send.at[k, planes], wf_recv.at[k, planes], dev(y_peer))
            for k, (a, c) in enumerate(zip(stage_refs(hi % 2), weight_refs(x_peer)))
        ]

    def start(copies):
        for copy in copies:
            copy.start()

    def wait_recv(copies):
        for copy in copies:
            copy.wait_recv()

    def wait_send(copies):
        for copy in copies:
            copy.wait_send()

    def relay_weights(i):
        for arrived, onward in zip(weight_copies(i), forward_copies(i)):
            arrived.wait_recv()
            onward.start()

    for d in range(1, planes):
        start(z_copies(d))
    start(first_copies(0))
    for i in range(1, planes):
        start(weight_copies(i))

    for a, b in zip(own_refs(s), weight_refs(s)):
        b[...] = a[...]
    for h in range(heads):
        turned_q[h] = turn(queries[:, h * head_size : (h + 1) * head_size], query_gain[...])
    peak[...] = jnp.full(peak.shape, -1e30, f32)
    total[...] = jnp.zeros(total.shape, f32)
    weighted[...] = jnp.zeros(weighted.shape, f32)
    exponent_scale = head_size ** (-0.5) * LOG2E

    def attend(slot):
        block_keys = key_buf[slot]
        block_values = value_buf[slot]
        for h in range(heads):
            scores = lax.dot_general(
                block_keys, turned_q[h], (((1,), (1,)), ((), ())), preferred_element_type=f32
            )
            old_peak = peak[h]
            new_peak = jnp.maximum(old_peak, jnp.max(scores, axis=0, keepdims=True))
            factor = jnp.exp2((old_peak - new_peak) * exponent_scale)
            raw = jnp.exp2((scores - new_peak) * exponent_scale)
            total[h] = total[h] * factor + jnp.sum(raw, axis=0, keepdims=True)
            weighted[h] = weighted[h] * factor + jnp.dot(
                block_values, raw.astype(bf16), preferred_element_type=f32
            )
            peak[h] = new_peak

    def first_step(d, carry):
        wait_recv(z_copies(d))
        start(first_copies(d))
        return carry

    def second_step(d, carry):
        wait_recv([first_copies(d)[0], first_copies(d)[1]])
        start(second_copies(d))
        return carry

    def attend_step(slot, carry):
        attend(slot)
        return carry

    attend(0)
    lax.fori_loop(1, planes, first_step, 0)
    start(stage_copies(0))
    start(stage_copies(1))
    lax.fori_loop(1, planes, attend_step, 0)
    lax.fori_loop(0, planes, second_step, 0)
    start(own_forward())

    def third_step(d, carry):
        first_copies(d)[3].wait_recv()
        attend(planes + d)
        return carry

    def fourth_step(d, carry):
        first_copies(d)[2].wait_recv()
        attend(2 * planes + d)

        @pl.when(d > 0)
        def _():
            relay_weights(d)

        return carry

    def fifth_step(d, carry):
        wait_recv(second_copies(d))
        attend(3 * planes + d)
        return carry

    lax.fori_loop(0, planes, third_step, 0)
    wait_recv(stage_copies(0))
    wait_recv(stage_copies(1))
    for d in range(1, planes):
        start(onward_copies(d))
    start(stage_forward())
    for a, b in zip(stage_refs(hi % 2), weight_refs(x_peer)):
        b[...] = a[...]
    lax.fori_loop(0, planes, fourth_step, 0)
    lax.fori_loop(0, planes, fifth_step, 0)
    for h in range(heads):
        attended[:, h * head_size : (h + 1) * head_size] = (weighted[h] / total[h]).T.astype(bf16)

    own_rows = pl.ds(pl.multiple_of(t * share, share), share)
    other_rows = pl.ds(pl.multiple_of((1 - t) * share, share), share)
    head_send[...] = jnp.dot(
        attended[other_rows, :], out_weight[...], preferred_element_type=f32
    ).astype(bf16)
    head_copy = remote(head_send, head_recv, h_send, h_recv, sibling)
    head_copy.start()
    head_own[...] = jnp.dot(
        attended[own_rows, :], out_weight[...], preferred_element_type=f32
    ).astype(bf16)
    head_copy.wait_recv()
    added = head_own[...].astype(f32) + head_recv[...].astype(f32)
    middle[...] = (residual_in[...].astype(f32) + added).astype(bf16)
    wide = middle[...].astype(f32)
    tokens[0, t] = (
        wide * lax.rsqrt(jnp.mean(wide * wide, axis=-1, keepdims=True) + EPS) * norm_gain[...]
    ).astype(bf16)

    def token_copy(r):
        return remote(
            tokens.at[0, t], tokens.at[r, t], t_send.at[0, r], t_recv.at[0, r], dev(member(r))
        )

    def sibling_copy(r):
        return remote(
            tokens.at[r, t], tokens.at[r, t], t_send.at[1, r], t_recv.at[1, r], sibling
        )

    def sibling_arrival(r):
        return remote(
            tokens.at[r, 1 - t], tokens.at[r, 1 - t], t_send.at[1, r], t_recv.at[1, r], sibling
        )

    for r in range(1, MEMBERS):
        token_copy(r).start()
    sibling_copy(0).start()

    def relay_step(d, carry):
        relay_weights(planes + d)
        return carry

    lax.fori_loop(1, planes, relay_step, 0)

    def arrivals(i):
        return [
            remote(a, a, wf_send.at[k, i], wf_recv.at[k, i], dev(y_peer))
            for k, a in enumerate(weight_refs(source_peer(i) + 2 - 4 * mid))
        ]

    def arrive_gate_up(i, carry):
        wait_recv(arrivals(i)[:2])
        return carry

    def arrive_down(i, carry):
        arrivals(i)[2].wait_recv()
        return carry

    lax.fori_loop(0, 2 * planes, arrive_gate_up, 0)

    def half_copy(r):
        return remote(
            half_send.at[r], half_recv.at[r], o_send.at[0, r], o_recv.at[0, r], sibling
        )

    def share_copy(r):
        return remote(
            share_send.at[r], share_recv.at[r], o_send.at[1, r], o_recv.at[1, r], dev(member(r))
        )

    def mix_rows(rows, tokens_half):
        both = jnp.dot(tokens_half, gate_up[...], preferred_element_type=f32)
        attended[rows, 0:part] = gated(both[:, :part], both[:, part:])

    def finish(r):
        half_copy(r).wait_recv()
        share_send[r] = (share_own[r] + half_recv[r].astype(f32)).astype(bf16)

    def mix_step(r, carry):
        @pl.when(r > 0)
        def _():
            token_copy(r).wait_recv()
            sibling_copy(r).start()

        mix_rows(own_rows, tokens[r, t])
        sibling_arrival(r).wait_recv()
        mix_rows(other_rows, tokens[r, 1 - t])

        @pl.when(r == 0)
        def _():
            lax.fori_loop(0, 2 * planes, arrive_down, 0)

        half_send[r] = jnp.dot(
            attended[other_rows, 0:part], down[...], preferred_element_type=f32
        ).astype(bf16)
        half_copy(r).start()
        share_own[r] = jnp.dot(attended[own_rows, 0:part], down[...], preferred_element_type=f32)

        @pl.when(r > 0)
        def _():
            finish(r)
            share_copy(r).start()

        return carry

    lax.fori_loop(0, MEMBERS, mix_step, 0)
    finish(0)
    out = middle[...].astype(f32) + share_send[0].astype(f32)
    for r in range(1, MEMBERS):
        share_copy(r).wait_recv()
        out = out + share_recv[r].astype(f32)
    result[...] = out.astype(bf16)

    for d in range(1, planes):
        wait_send(z_copies(d))
    for d in range(planes):
        wait_send(first_copies(d))
        wait_send(second_copies(d))
    wait_send(own_forward())
    for b in range(2):
        wait_send(stage_copies(b))
    wait_send(stage_forward())
    for d in range(1, planes):
        wait_send(weight_copies(d))
        wait_send(onward_copies(d))
        wait_send(forward_copies(d))
        wait_send(forward_copies(planes + d))
    head_copy.wait_send()
    for r in range(MEMBERS):
        sibling_copy(r).wait_send()
        half_copy(r).wait_send()
        if r > 0:
            token_copy(r).wait_send()
            share_copy(r).wait_send()


def fused(
    queries, keys, values, query_gain, key_gain, residual_in, out_weight, norm_gain,
    gate_weight, up_weight, down_weight,
):
    n_sp = lax.axis_size("sp")
    planes = n_sp // 4
    tok_rows, width = queries.shape
    head_size = query_gain.shape[0]
    heads = width // head_size
    share, model = residual_in.shape
    depth, part = gate_weight.shape[0], gate_weight.shape[1] // MEMBERS
    f32, bf16 = jnp.float32, jnp.bfloat16
    cosine, sine = rotary_tables(tok_rows, head_size)
    vmem = pl.BlockSpec(memory_space=pltpu.VMEM)
    dma = pltpu.SemaphoreType.DMA
    return pl.pallas_call(
        functools.partial(layer_kernel, n_sp),
        out_shape=jax.ShapeDtypeStruct((share, model), bf16),
        in_specs=[vmem] * 13,
        out_specs=vmem,
        scratch_shapes=[
            pltpu.VMEM((heads, tok_rows, head_size), bf16),
            pltpu.VMEM((n_sp, tok_rows, head_size), bf16),
            pltpu.VMEM((n_sp, head_size, tok_rows), bf16),
            pltpu.VMEM((heads, 1, tok_rows), f32),
            pltpu.VMEM((heads, 1, tok_rows), f32),
            pltpu.VMEM((heads, head_size, tok_rows), f32),
            pltpu.VMEM((tok_rows, max(width, part)), bf16),
            pltpu.VMEM((share, model), bf16),
            pltpu.VMEM((share, model), bf16),
            pltpu.VMEM((share, model), bf16),
            pltpu.VMEM((share, model), bf16),
            pltpu.VMEM((MEMBERS, 2, share, model), bf16),
            pltpu.VMEM((model, 2 * part), bf16),
            pltpu.VMEM((part, model), bf16),
            pltpu.VMEM((2, depth, 2 * part), bf16),
            pltpu.VMEM((2, part, depth), bf16),
            pltpu.VMEM((MEMBERS, share, model), bf16),
            pltpu.VMEM((MEMBERS, share, model), bf16),
            pltpu.VMEM((MEMBERS, share, model), bf16),
            pltpu.VMEM((MEMBERS, share, model), bf16),
            pltpu.VMEM((MEMBERS, share, model), f32),
            dma((2, 3, n_sp)),
            dma((2, n_sp)),
            dma((3, 2 * planes)),
            dma((3, 2 * planes)),
            dma((3, 2 * planes)),
            dma((3, 2 * planes)),
            dma((3, 2)),
            dma((3, 2)),
            dma,
            dma,
            dma((2, MEMBERS)),
            dma((2, MEMBERS)),
            dma((2, MEMBERS)),
            dma((2, MEMBERS)),
        ],
        compiler_params=pltpu.CompilerParams(
            collective_id=0, has_side_effects=True, vmem_limit_bytes=60 * 1024 * 1024
        ),
    )(
        queries, keys, values, query_gain.reshape(1, -1), key_gain.reshape(1, -1), residual_in,
        out_weight, norm_gain.reshape(1, -1), gate_weight, up_weight, down_weight, cosine, sine,
    )


def layer(*args):
    queries, residual_in, gate_weight = args[0], args[5], args[8]
    head_size = args[3].shape[0]
    fits = (
        lax.axis_size("sp") % 8 == 0
        and lax.axis_size("tp") == 2
        and residual_in.shape[0] * 2 == queries.shape[0]
        and residual_in.shape[0] % 16 == 0
        and head_size == 128
        and queries.shape[1] % head_size == 0
        and gate_weight.shape[0] % 128 == 0
        and gate_weight.shape[1] % (128 * MEMBERS) == 0
        and (Q_HEADS // KV_HEADS) % (queries.shape[1] // head_size) == 0
    )
    return fused(*args) if fits else local(*args)


def solution(mesh):
    return jax.shard_map(
        layer,
        mesh=mesh,
        in_specs=(
            P("sp", "tp"),
            P("sp", None),
            P("sp", None),
            P(),
            P(),
            P(("sp", "tp"), None),
            P("tp", None),
            P(),
            P("sp", "tp"),
            P("sp", "tp"),
            P("tp", "sp"),
        ),
        out_specs=P(("sp", "tp"), None),
        check_vma=False,
    )
```
